32 devices in a mesh: sp: 4 (over y, x), tp: 8 (over z, core).
Axes of the slice: x: 2, y: 2, z: 4, core: 2. Of those that a mesh axis runs over, the one named last changes fastest.
Arguments:
- query_input: bfloat16 [1024, 1024], P('tp', 'sp'), may hold values from -6 to 6
- key_input: bfloat16 [1024, 1024], P('tp', 'sp'), may hold values from -6 to 6
- retrieved_content_matrix: bfloat16 [1024, 1024], P('tp', 'sp'), may hold values from -6 to 6
- gate_input: bfloat16 [1024, 1024], P('tp', 'sp'), may hold values from -6 to 6
- log_decay: float32 [2, 16, 1024], P(None, 'tp', 'sp'), may hold values from -2 to 0
- residual: bfloat16 [1024, 2048], P(('sp', 'tp')), may hold values from -6 to 6
- out_weight: bfloat16 [1024, 2048], replicated, may hold values from -0.1875 to 0.1875
- norm_gain: bfloat16 [2048], replicated, may hold values from 0.099609375 to 1.8984375
- routes: int32 [1024, 2], P(('sp', 'tp')), may hold values from 0 to 3, all different within a row; in each aligned block of 32 rows (0 to 31, 32 to 63, ...) at most 20 rows name the same one
- route_weight: float32 [1024, 2], P(('sp', 'tp')), may hold values from 0.1 to 1
- gate_weight: bfloat16 [4, 2048, 5504], P('sp', None, 'tp'), may hold values from -0.125 to 0.125
- up_weight: bfloat16 [4, 2048, 5504], P('sp', None, 'tp'), may hold values from -0.125 to 0.125
- down_weight: bfloat16 [4, 5504, 2048], P('sp', 'tp'), may hold values from -0.078125 to 0.078125
Outputs:
- output: bfloat16 [1024, 2048], P(('sp', 'tp'))
The draws below stay inside these ranges and needn't reach their ends.
Inputs may be any that keep to these rules, and one draw needn't show every extreme that they name: `routes`: each row names 2 different experts. In each aligned block of 32 rows no expert is named by more than 20 rows, a bound that some block reaches.
All inputs are finite; a program needn't handle non-finite values.
Results may differ from the reference program's by a relative error of at most 0.015.
Values may be sent and summed in bfloat16 or wider, within the bound.
No kernel may reach another device: no remote copies, remote signals or barrier semaphores. Data moves between devices by JAX's collectives and lax.ppermute only.
A program may use at most 64 MiB of HBM per device.

```python
import math
import jax
import jax.numpy as jnp
import numpy as np
from jax import lax

D = 2048
HEADS = 16
HEAD_DIM = 64
RET_W = 1024
FF = 5504
FF_DEV = 688
EXPERTS = 4
TOP = 2
TOK_DEV = 256
TOK_TP = 32
TOKENS = 1024
CAP = 20
N_TP = 8


def draw_log_decay(key, part):
    streams = jax.random.split(key, 9)
    blocks = TOKENS // TOK_DEV
    sluggish_tally = HEADS // 2
    order_forward = jax.random.permutation(streams[0], HEADS)
    order_backward = jax.random.permutation(streams[1], HEADS)
    slow = jnp.stack([order_forward < sluggish_tally, order_backward < sluggish_tally])
    slow_rate = jax.random.uniform(streams[2], (2, HEADS), jnp.float32, 0.15, 0.4) / TOKENS
    fast_rate = jax.random.uniform(streams[3], (2, HEADS), jnp.float32, 0.015, 0.03)
    rate = jnp.where(slow, slow_rate, fast_rate)
    parity = jax.random.randint(streams[4], (), 0, 2)
    signs = jnp.where((jnp.arange(blocks) + parity) % 2 == 0, 1.0, -1.0)
    levels = jax.random.uniform(streams[5], (2, 1, blocks), jnp.float32, 0.5, 1.0)
    factor = jnp.repeat(jnp.exp2(signs[None, None, :] * levels), TOK_DEV, axis=2)
    rough = jax.random.uniform(streams[6], (2, HEADS, TOKENS), jnp.float32, 0.5, 1.5)
    starting_displacement = -rate[:, :, None] * factor * rough
    bucket_locations = jax.random.randint(streams[7], (2, HEADS, 2), 0, TOKENS)
    portion_quantities = jax.random.uniform(streams[8], (2, HEADS, 2), jnp.float32, math.log(0.5), math.log(0.8))
    element_locations = jnp.arange(TOKENS)
    element_runs = jnp.sum(jnp.where(element_locations[None, None, None, :] == bucket_locations[..., None], portion_quantities[..., None], 0.0), axis=2)
    return (starting_displacement + element_runs).astype(jnp.float32)


def level_of(key, dims, shards, least, largest):
    loudness, own = 1.0, jax.random.fold_in(key, 6)
    for dim, shards_of in shards:
        steps = jnp.exp(jax.random.uniform(jax.random.fold_in(own, dim), (shards_of,), jnp.float32, least / len(shards), largest / len(shards)))
        loudness = loudness * jnp.repeat(steps, dims[dim] // shards_of).reshape([-1 if axis == dim else 1 for axis in range(len(dims))])
    return loudness


def assign_block(own_key, own, number, rows, number_of, top, most, lean):
    order = jax.random.permutation(own_key, number_of)
    crowded, usual = portions_of(number_of, rows * top, most, lean, True), portions_of(number_of, rows * top, most, lean, False)
    places = jnp.arange(number_of)

    def named(sizes, rotation):
        used = int((sizes > 0).sum())
        fixed = max(1, used // 4)
        shifted = fixed + (places - fixed + rotation * (used - fixed)) % max(1, number_of - fixed)
        return jnp.zeros((number_of,), jnp.int32).at[order[jnp.where(places < fixed, places, shifted)]].set(jnp.asarray(sizes, jnp.int32))

    sizes = jnp.where(number % 4 == 0, named(crowded, number // 4), named(usual, number - number // 4 - 1))
    mixed = jax.random.permutation(jax.random.fold_in(own, 3), number_of)
    giver, receiver = mixed[0:number_of // 2 * 2:2], mixed[1:number_of // 2 * 2:2]
    margin = jnp.minimum(sizes[giver] - 1, most - sizes[receiver]) // 2
    margin = jnp.where((giver == order[0]) | (receiver == order[0]) | (sizes[receiver] == 0), 0, jnp.maximum(margin, 0))
    shifted = jax.random.randint(jax.random.fold_in(own, 4), (number_of // 2,), 0, 1 << 20) % (margin + 1)
    sizes = sizes.at[giver].add(-shifted).at[receiver].add(shifted)
    members = jnp.searchsorted(jnp.cumsum(sizes), jnp.arange(rows * top), side="right").astype(jnp.int32)
    table = members.reshape(top, rows).T
    table = table[jax.random.permutation(jax.random.fold_in(own, 1), rows)]
    rotation = jax.random.randint(jax.random.fold_in(own, 2), (rows, 1), 0, top)
    return jnp.take_along_axis(table, (jnp.arange(top)[None, :] + rotation) % top, axis=1)


def portions_of(count, total, reach, lean, full):
    loads = [(1 << 20) // math.isqrt(standing ** lean) + 1 for standing in range(1, count + 1)]
    largest = reach if full else min(reach, max(-(-total // count), total * loads[0] // sum(loads)))
    least = 1 if total - largest >= count - 1 else 0
    counts, surplus = [largest] + [least] * (count - 1), total - largest - least * (count - 1)
    while surplus > 0:
        candidates = [i for i in range(1, count) if counts[i] < largest] or [i for i in range(1, count) if counts[i] < reach]
        pool, budget = sum([loads[i] for i in candidates]), surplus
        for i in candidates:
            extra = min(reach - counts[i], max(1, budget * loads[i] // pool), surplus)
            counts[i] = counts[i] + extra
            surplus = surplus - extra
    return np.array(counts)


def gaussian(stream_key, extent, spread, limit, shards=(), held_as=jnp.bfloat16):
    result = jax.random.normal(stream_key, extent, jnp.float32) * spread
    if len(shards) > 0:
        result = level_of(stream_key, extent, shards, -0.22, 0.18) * result
    return jnp.clip(result, min=-limit, max=limit).astype(held_as)


def setup_inputs(seed: int = 0) -> dict:
    splits = jax.random.split(jax.random.key(seed), 14)
    query_input = gaussian(splits[0], (RET_W, TOKENS), 1.0, 6.0, ((0, 8), (1, 4)))
    key_input = gaussian(splits[1], (RET_W, TOKENS), 1.0, 6.0, ((0, 8), (1, 4)))
    retrieved_content_matrix = gaussian(splits[2], (RET_W, TOKENS), 1.0, 6.0, ((0, 8), (1, 4)))
    gate_input = gaussian(splits[3], (RET_W, TOKENS), 1.0, 6.0, ((0, 8), (1, 4)))
    log_decay = draw_log_decay(jax.random.fold_in(splits[13], 71), 0)
    residual = gaussian(splits[5], (TOKENS, D), 1.0, 6.0, ((0, 32),))
    out_weight = gaussian(splits[6], (RET_W, D), RET_W ** -0.5, 0.1875)
    norm_gain = jnp.clip(1.0 + 0.18 * jax.random.normal(splits[7], (D,), jnp.float32), 0.099609375, 1.8984375).astype(jnp.bfloat16)
    routes_keys = jax.random.split(jax.random.fold_in(splits[8], 1), TOKENS // TOK_TP)
    routes_turns = jax.random.permutation(jax.random.fold_in(splits[8], 3), TOKENS // TOK_TP)
    routes = jax.vmap(lambda own, number: assign_block(jax.random.fold_in(splits[8], 2), own, number, TOK_TP, EXPERTS, TOP, CAP, 1))(routes_keys, routes_turns).reshape((TOKENS, TOP))
    route_weight = jnp.clip(0.1 + 0.9 * jax.random.uniform(splits[9], (TOKENS, TOP), jnp.float32) ** level_of(splits[9], (TOKENS, TOP), ((0, 32),), -0.2, 0.2), 0.1, 1.0)
    gate_weight = gaussian(splits[10], (EXPERTS, D, FF), D ** -0.5, 0.125, ((0, 4), (2, 8)))
    up_weight = gaussian(splits[11], (EXPERTS, D, FF), D ** -0.5, 0.125, ((0, 4), (2, 8)))
    down_weight = gaussian(splits[12], (EXPERTS, FF, D), FF ** -0.5, 0.078125, ((0, 4), (1, 8)))
    return {"query_input": query_input, "key_input": key_input, "retrieved_content_matrix": retrieved_content_matrix, "gate_input": gate_input, "log_decay": log_decay, "residual": residual, "out_weight": out_weight, "norm_gain": norm_gain, "routes": routes, "route_weight": route_weight, "gate_weight": gate_weight, "up_weight": up_weight, "down_weight": down_weight}


full_precision = lax.Precision.HIGHEST

def head_norm(values, mesh_axis):
    centred = values - lax.optimization_barrier(jnp.mean(values, axis=mesh_axis, keepdims=True))
    return centred * lax.rsqrt(lax.optimization_barrier(jnp.mean(centred * centred, axis=mesh_axis, keepdims=True)) + 1e-06)

def reference(query_input, key_input, retrieved_content_matrix, gate_input, log_decay, residual, out_weight, norm_gain, routes, route_weight, gate_weight, up_weight, down_weight):
    segment_count = TOKENS // TOK_DEV

    def by_segment(array):
        shaped = array.astype(jnp.float32).reshape(HEADS, HEAD_DIM, segment_count, TOK_DEV)
        return jnp.transpose(shaped, (2, 0, 1, 3))
    queries = by_segment(query_input)
    all_keys = by_segment(key_input)
    all_values = by_segment(retrieved_content_matrix)
    gate_values = by_segment(gate_input)
    forward_log = jnp.transpose(log_decay[0].reshape(HEADS, segment_count, TOK_DEV), (1, 0, 2))
    backward_log = jnp.transpose(log_decay[1].reshape(HEADS, segment_count, TOK_DEV), (1, 0, 2))
    forward_prefix = jnp.cumsum(forward_log, axis=-1)
    backward_prefix = jnp.cumsum(backward_log, axis=-1) - backward_log
    forward_total = forward_prefix[..., -1]
    backward_total = lax.optimization_barrier(jnp.sum(backward_log, axis=-1))
    forward_keys = all_keys * jnp.exp(forward_total[..., None] - forward_prefix)[:, :, None, :]
    backward_keys = all_keys * jnp.exp(backward_prefix)[:, :, None, :]
    local_forward = jnp.einsum('nhds,nhes->nhde', forward_keys, all_values, precision=full_precision)
    backward_local = jnp.einsum('nhds,nhes->nhde', backward_keys, all_values, precision=full_precision)

    def carry_step(state, inputs):
        total, local = inputs
        return (jnp.exp(total)[:, None, None] * state + local, state)
    zero_state = jnp.zeros((HEADS, HEAD_DIM, HEAD_DIM), jnp.float32)
    _, forward_in = lax.scan(carry_step, zero_state, (forward_total, local_forward))
    _, backward_in = lax.scan(carry_step, zero_state, (backward_total, backward_local), reverse=True)
    offsets = jnp.arange(TOK_DEV)
    lower = offsets[:, None] >= offsets[None, :]
    upper = offsets[:, None] <= offsets[None, :]

    def segment_output(inputs):
        query_part, key_part, value_part, forward_part, backward_part, backward_sum, state_fwd, state_bwd = inputs
        scores = jnp.einsum('hdt,hds->hts', query_part, key_part)
        forward_decay_weight = jnp.exp(jnp.where(lower, forward_part[:, :, None] - forward_part[:, None, :], -jnp.inf))
        backward_weight = jnp.exp(jnp.where(upper, backward_part[:, None, :] - backward_part[:, :, None], -jnp.inf))
        weighted = (scores * (forward_decay_weight + backward_weight)).astype(jnp.bfloat16)
        weighted = lax.optimization_barrier(weighted).astype(jnp.float32)
        inner = jnp.einsum('hts,hes->het', weighted, value_part)
        carried = jnp.einsum('hdt,hde->het', query_part, state_fwd, precision=full_precision) * jnp.exp(forward_part)[:, None, :]
        carried = carried + jnp.einsum('hdt,hde->het', query_part, state_bwd, precision=full_precision) * jnp.exp(backward_sum[:, None] - backward_part)[:, None, :]
        return inner + carried
    retained = lax.map(segment_output, (queries, all_keys, all_values, forward_prefix, backward_prefix, backward_total, forward_in, backward_in))
    mixer_out = (head_norm(retained, 2) * jax.nn.silu(gate_values)).astype(jnp.bfloat16)
    mixer_tokens = jnp.transpose(mixer_out, (0, 3, 1, 2)).reshape(TOKENS, RET_W)
    stream = residual.astype(jnp.float32) + jnp.dot(mixer_tokens, out_weight, preferred_element_type=jnp.float32)
    scale = lax.rsqrt(lax.optimization_barrier(jnp.mean(stream * stream, axis=-1, keepdims=True)) + 1e-06)
    normed = (stream * scale * norm_gain.astype(jnp.float32)).astype(jnp.bfloat16)
    slots_total = CAP * (TOKENS // TOK_TP)

    def expert_step(expert, moe_sum):
        chosen = jnp.any(routes == expert, axis=-1)
        picked = jnp.nonzero(chosen, size=slots_total, fill_value=0)[0].astype(jnp.int32)
        valid = (jnp.arange(slots_total) < jnp.sum(chosen.astype(jnp.int32))).astype(jnp.float32)
        inputs = normed[picked]
        gates = jnp.dot(inputs, gate_weight[expert], preferred_element_type=jnp.float32)
        ups = jnp.dot(inputs, up_weight[expert], preferred_element_type=jnp.float32)
        hidden = (jax.nn.silu(gates) * ups).astype(jnp.bfloat16)
        grouped = hidden.reshape(slots_total, N_TP, FF_DEV).astype(jnp.float32)
        down_groups = down_weight[expert].reshape(N_TP, FF_DEV, D).astype(jnp.float32)
        parts = jnp.einsum('rjf,jfd->rjd', grouped, down_groups).astype(jnp.bfloat16)
        parts = lax.optimization_barrier(parts).astype(jnp.float32)
        expert_out = lax.optimization_barrier(jnp.sum(parts, axis=1)).astype(jnp.bfloat16)
        weight = lax.optimization_barrier(jnp.sum(jnp.where(routes[picked] == expert, route_weight[picked], 0.0), axis=-1)) * valid
        return moe_sum.at[picked].add(weight[:, None] * expert_out.astype(jnp.float32))
    moe_sum = lax.fori_loop(0, EXPERTS, expert_step, jnp.zeros((TOKENS, D), jnp.float32))
    return (stream + moe_sum).astype(jnp.bfloat16)
```

```python
import jax
import jax.numpy as jnp
from jax import lax
from jax.sharding import PartitionSpec as P

HEAD_DIM = 64

full_precision = lax.Precision.HIGHEST


def rotate(value, axis, step):
    count = lax.axis_size(axis)
    return lax.ppermute(value, axis, [(i, (i + step) % count) for i in range(count)])


def swap_core(value):
    return lax.ppermute(value, "tp", [(i, i ^ 1) for i in range(lax.axis_size("tp"))])


def head_norm(values, mesh_axis):
    centred = values - jnp.mean(values, axis=mesh_axis, keepdims=True)
    return centred * lax.rsqrt(jnp.mean(centred * centred, axis=mesh_axis, keepdims=True) + 1e-06)


def exchange_states(forward_total, forward_local, backward_total, backward_local):
    count, mine = lax.axis_size("sp"), lax.axis_index("sp")

    def packed(total, local):
        return jnp.concatenate(
            [local, jnp.broadcast_to(total[:, None, None], (local.shape[0], 8, local.shape[2]))], axis=1
        )

    ahead = packed(forward_total, forward_local)
    behind = packed(backward_total, backward_local)
    got = {}
    for step in range(1, count):
        got[step] = rotate(jnp.where(mine + step < count, ahead, behind), "sp", step)

    def joined(distances):
        state = jnp.zeros_like(forward_local)
        between = jnp.zeros_like(forward_total)
        for piece, valid in distances:
            state = state + jnp.where(
                valid, jnp.exp(between)[:, None, None] * piece[:, :HEAD_DIM], 0.0
            )
            between = between + jnp.where(valid, piece[:, HEAD_DIM, 0], 0.0)
        return state

    forward_in = joined([(got[d], mine >= d) for d in range(1, count)])
    backward_in = joined([(got[count - d], mine + d < count) for d in range(1, count)])
    return forward_in, backward_in


def mixer(query_input, key_input, retrieved_content_matrix, gate_input, log_decay):
    heads_here = query_input.shape[0] // HEAD_DIM
    length = query_input.shape[1]
    queries = query_input.reshape(heads_here, HEAD_DIM, length)
    all_keys = key_input.reshape(heads_here, HEAD_DIM, length)
    all_values = retrieved_content_matrix.reshape(heads_here, HEAD_DIM, length)
    forward_log = log_decay[0]
    backward_log = log_decay[1]
    forward_prefix = jnp.cumsum(forward_log, axis=-1)
    backward_prefix = jnp.cumsum(backward_log, axis=-1) - backward_log
    forward_total = forward_prefix[:, -1]
    backward_total = jnp.sum(backward_log, axis=-1)
    wide_keys = all_keys.astype(jnp.float32)
    wide_values = all_values.astype(jnp.float32)
    forward_keys = wide_keys * jnp.exp(forward_total[:, None] - forward_prefix)[:, None, :]
    backward_keys = wide_keys * jnp.exp(backward_prefix)[:, None, :]
    local_forward = jnp.einsum("hds,hes->hde", forward_keys, wide_values, precision=full_precision)
    backward_local = jnp.einsum(
        "hds,hes->hde", backward_keys, wide_values, precision=full_precision
    )
    forward_in, backward_in = exchange_states(
        forward_total, local_forward, backward_total, backward_local
    )
    offsets = jnp.arange(length)
    scores = jnp.einsum("hdt,hds->hts", queries, all_keys, preferred_element_type=jnp.float32)
    gap = jnp.where(
        (offsets[:, None] >= offsets[None, :])[None],
        forward_prefix[:, :, None] - forward_prefix[:, None, :],
        backward_prefix[:, None, :] - backward_prefix[:, :, None],
    )
    decay = jnp.exp(gap) * jnp.where(offsets[:, None] == offsets[None, :], 2.0, 1.0)[None]
    weighted = (scores * decay).astype(jnp.bfloat16)
    inner = jnp.einsum("hts,hes->het", weighted, all_values, preferred_element_type=jnp.float32)
    query_wide = queries.astype(jnp.float32)
    both_queries = jnp.concatenate(
        [
            query_wide * jnp.exp(forward_prefix)[:, None, :],
            query_wide * jnp.exp(backward_total[:, None] - backward_prefix)[:, None, :],
        ],
        axis=1,
    )
    both_states = jnp.concatenate([forward_in, backward_in], axis=1)
    carried = jnp.einsum("hdt,hde->het", both_queries, both_states, precision=full_precision)
    retained = inner + carried
    gate_values = gate_input.reshape(heads_here, HEAD_DIM, length).astype(jnp.float32)
    return (
        (head_norm(retained, 1) * jax.nn.silu(gate_values))
        .reshape(heads_here * HEAD_DIM, length)
        .astype(jnp.bfloat16)
    )


def split_float(value):
    high = lax.reduce_precision(value, 8, 7)
    middle = lax.reduce_precision(value - high, 8, 7)
    low = value - high - middle
    return high, middle, low


def on_device(
    query_input,
    key_input,
    retrieved_content_matrix,
    gate_input,
    log_decay,
    residual,
    out_weight,
    norm_gain,
    routes,
    route_weight,
    gate_weight,
    up_weight,
    down_weight,
):
    groups, mine = lax.axis_size("sp"), lax.axis_index("sp")
    chips = lax.axis_size("tp") // 2
    mixer_out = mixer(query_input, key_input, retrieved_content_matrix, gate_input, log_decay)
    token_major = lax.all_to_all(mixer_out, "tp", split_axis=1, concat_axis=0, tiled=True)
    projected = lax.dot_general(
        token_major, out_weight, (((0,), (0,)), ((), ())), preferred_element_type=jnp.float32
    )
    stream = residual.astype(jnp.float32) + projected
    scale = lax.rsqrt(jnp.mean(stream * stream, axis=-1, keepdims=True) + 1e-06)
    normed = (stream * scale * norm_gain.astype(jnp.float32)).astype(jnp.bfloat16)
    token_count, picks = routes.shape
    width = normed.shape[1]
    experts_all = groups * gate_weight.shape[0]
    capacity = (5 * token_count + 2 * experts_all - 1) // (2 * experts_all)

    side = jnp.concatenate([routes.astype(jnp.float32), *split_float(route_weight)], axis=1)
    side = jnp.pad(side.astype(jnp.bfloat16), ((0, 0), (0, 128 - side.shape[1])))
    message = jnp.concatenate([normed, side], axis=1)
    pieces = [message] + [rotate(message, "tp", 2 * step) for step in range(1, chips)]
    tokens = jnp.concatenate(pieces, axis=0)
    rows = tokens[:, :width]
    side_all = tokens[:, width:].astype(jnp.float32)
    routes_all = side_all[:, :picks].astype(jnp.int32)
    weights_all = (
        side_all[:, picks : 2 * picks]
        + side_all[:, 2 * picks : 3 * picks]
        + side_all[:, 3 * picks : 4 * picks]
    )
    relative = (routes_all - mine) % groups
    blocked = relative.reshape(chips, token_count * picks)
    matches = (blocked[:, :, None] == jnp.arange(groups)[None, None, :]).astype(jnp.float32)
    slots_before = jnp.arange(token_count * picks)
    earlier = (slots_before[:, None] > slots_before[None, :]).astype(jnp.float32)
    ranks = jnp.einsum("ij,bjg->big", earlier, matches)
    rank = jnp.sum(ranks * matches, axis=2).astype(jnp.int32)
    target = blocked * (chips * capacity) + jnp.arange(chips)[:, None] * capacity + rank
    target = target.reshape(chips * token_count, picks)
    slot_grid = jnp.arange(groups * chips * capacity)
    hits = slot_grid[:, None, None] == target[None, :, :]
    placing = jnp.sum(hits.astype(jnp.float32), axis=2).astype(jnp.bfloat16)
    gathering = jnp.sum(jnp.where(hits, weights_all[None], 0.0), axis=2)
    send_rows = jnp.dot(placing, rows, preferred_element_type=jnp.float32).astype(jnp.bfloat16)
    send_rows = send_rows.reshape(groups, chips * capacity, width)
    received = [send_rows[0]] + [rotate(send_rows[step], "sp", step) for step in range(1, groups)]
    own_half = jnp.concatenate(received, axis=0)
    other_half = swap_core(own_half)

    def expert(flat_rows):
        gates = jnp.dot(flat_rows, gate_weight[0], preferred_element_type=jnp.float32)
        ups = jnp.dot(flat_rows, up_weight[0], preferred_element_type=jnp.float32)
        hidden = (jax.nn.silu(gates) * ups).astype(jnp.bfloat16)
        return jnp.dot(hidden, down_weight[0], preferred_element_type=jnp.float32)

    own_part = expert(own_half)
    other_part = swap_core(expert(other_half).astype(jnp.bfloat16))
    summed = (own_part + other_part.astype(jnp.float32)).astype(jnp.bfloat16)
    summed = summed.reshape(groups, chips * capacity, width)
    returned = [summed[0]] + [rotate(summed[step], "sp", -step) for step in range(1, groups)]
    flat_back = jnp.concatenate(returned, axis=0)
    high, middle, _ = split_float(gathering)
    combined = lax.dot_general(
        jnp.concatenate([high, middle], axis=0).astype(jnp.bfloat16),
        jnp.concatenate([flat_back, flat_back], axis=0),
        (((0,), (0,)), ((), ())),
        preferred_element_type=jnp.float32,
    )
    combined = combined.reshape(chips, token_count, width)
    result = stream + combined[0]
    for step in range(1, chips):
        result = result + rotate(
            combined[step].astype(jnp.bfloat16), "tp", -2 * step
        ).astype(jnp.float32)
    return result.astype(jnp.bfloat16)


def solution(mesh):
    placed = (
        P("tp", "sp"),
        P("tp", "sp"),
        P("tp", "sp"),
        P("tp", "sp"),
        P(None, "tp", "sp"),
        P(("sp", "tp"), None),
        P(),
        P(),
        P(("sp", "tp"), None),
        P(("sp", "tp"), None),
        P("sp", None, "tp"),
        P("sp", None, "tp"),
        P("sp", "tp", None),
    )
    return jax.shard_map(
        on_device, mesh=mesh, in_specs=placed, out_specs=P(("sp", "tp"), None), check_vma=False
    )
```

```python
import jax
import jax.numpy as jnp
from jax import lax
from jax.experimental import pallas as pl
from jax.experimental.layout import Layout, with_layout_constraint
from jax.experimental.pallas import tpu as pltpu
from jax.sharding import PartitionSpec as P

HEAD_DIM = 64

full_precision = lax.Precision.HIGHEST


def rotate(value, axis, step):
    count = lax.axis_size(axis)
    return lax.ppermute(value, axis, [(i, (i + step) % count) for i in range(count)])


def row_major(value):
    return with_layout_constraint(value, Layout(major_to_minor=tuple(range(value.ndim))))


def expert_body(rows, gate, up, down, out):
    last = (((1,), (1,)), ((), ()))
    gates = lax.dot_general(rows[...], gate[...], last, preferred_element_type=jnp.float32)
    ups = lax.dot_general(rows[...], up[...], last, preferred_element_type=jnp.float32)
    hidden = (gates * jax.nn.sigmoid(gates) * ups).astype(jnp.bfloat16)
    out[...] = jnp.dot(hidden, down[...], preferred_element_type=jnp.float32).astype(out.dtype)


def expert_kernel(rows, gate, up, down):
    space = pl.BlockSpec(memory_space=pltpu.VMEM)
    return pl.pallas_call(
        expert_body,
        out_shape=jax.ShapeDtypeStruct((rows.shape[0], down.shape[1]), jnp.bfloat16),
        in_specs=[space] * 4,
        out_specs=space,
        compiler_params=pltpu.CompilerParams(vmem_limit_bytes=48 * 1024 * 1024),
        name="expert",
    )(rows, gate, up, down)


def swap_core(value):
    return lax.ppermute(value, "tp", [(i, i ^ 1) for i in range(lax.axis_size("tp"))])


def head_norm(values, mesh_axis):
    centred = values - jnp.mean(values, axis=mesh_axis, keepdims=True)
    return centred * lax.rsqrt(jnp.mean(centred * centred, axis=mesh_axis, keepdims=True) + 1e-06)


def exchange_states(forward_total, forward_local, backward_total, backward_local):
    count, mine = lax.axis_size("sp"), lax.axis_index("sp")

    def packed(total, local):
        return jnp.concatenate(
            [local, jnp.broadcast_to(total[:, None, None], (local.shape[0], 8, local.shape[2]))], axis=1
        )

    ahead = packed(forward_total, forward_local)
    behind = packed(backward_total, backward_local)
    got = {}
    for step in range(1, count):
        got[step] = rotate(jnp.where(mine + step < count, ahead, behind), "sp", step)

    def joined(distances):
        state = jnp.zeros_like(forward_local)
        between = jnp.zeros_like(forward_total)
        for piece, valid in distances:
            state = state + jnp.where(
                valid, jnp.exp(between)[:, None, None] * piece[:, :HEAD_DIM], 0.0
            )
            between = between + jnp.where(valid, piece[:, HEAD_DIM, 0], 0.0)
        return state

    forward_in = joined([(got[d], mine >= d) for d in range(1, count)])
    backward_in = joined([(got[count - d], mine + d < count) for d in range(1, count)])
    return forward_in, backward_in


def mixer(query_input, key_input, retrieved_content_matrix, gate_input, log_decay):
    heads_here = query_input.shape[0] // HEAD_DIM
    length = query_input.shape[1]
    queries = query_input.reshape(heads_here, HEAD_DIM, length)
    all_keys = key_input.reshape(heads_here, HEAD_DIM, length)
    all_values = retrieved_content_matrix.reshape(heads_here, HEAD_DIM, length)
    forward_log = log_decay[0]
    backward_log = log_decay[1]
    forward_prefix = jnp.cumsum(forward_log, axis=-1)
    backward_prefix = jnp.cumsum(backward_log, axis=-1) - backward_log
    forward_total = forward_prefix[:, -1]
    backward_total = jnp.sum(backward_log, axis=-1)
    wide_keys = all_keys.astype(jnp.float32)
    wide_values = all_values.astype(jnp.float32)
    forward_keys = wide_keys * jnp.exp(forward_total[:, None] - forward_prefix)[:, None, :]
    backward_keys = wide_keys * jnp.exp(backward_prefix)[:, None, :]
    local_forward = jnp.einsum("hds,hes->hde", forward_keys, wide_values, precision=full_precision)
    backward_local = jnp.einsum(
        "hds,hes->hde", backward_keys, wide_values, precision=full_precision
    )
    forward_in, backward_in = exchange_states(
        forward_total, local_forward, backward_total, backward_local
    )
    offsets = jnp.arange(length)
    scores = jnp.einsum("hdt,hds->hts", queries, all_keys, preferred_element_type=jnp.float32)
    gap = jnp.where(
        (offsets[:, None] >= offsets[None, :])[None],
        forward_prefix[:, :, None] - forward_prefix[:, None, :],
        backward_prefix[:, None, :] - backward_prefix[:, :, None],
    )
    decay = jnp.exp(gap) * jnp.where(offsets[:, None] == offsets[None, :], 2.0, 1.0)[None]
    weighted = (scores * decay).astype(jnp.bfloat16)
    inner = jnp.einsum("hts,hes->het", weighted, all_values, preferred_element_type=jnp.float32)
    query_wide = queries.astype(jnp.float32)
    both_queries = jnp.concatenate(
        [
            query_wide * jnp.exp(forward_prefix)[:, None, :],
            query_wide * jnp.exp(backward_total[:, None] - backward_prefix)[:, None, :],
        ],
        axis=1,
    )
    both_states = jnp.concatenate([forward_in, backward_in], axis=1)
    carried = jnp.einsum("hdt,hde->het", both_queries, both_states, precision=full_precision)
    retained = inner + carried
    gate_values = gate_input.reshape(heads_here, HEAD_DIM, length).astype(jnp.float32)
    return (
        (head_norm(retained, 1) * jax.nn.silu(gate_values))
        .reshape(heads_here * HEAD_DIM, length)
        .astype(jnp.bfloat16)
    )


def split_float(value):
    high = lax.reduce_precision(value, 8, 7)
    middle = lax.reduce_precision(value - high, 8, 7)
    low = value - high - middle
    return high, middle, low


def on_device(
    query_input,
    key_input,
    retrieved_content_matrix,
    gate_input,
    log_decay,
    residual,
    out_weight,
    norm_gain,
    routes,
    route_weight,
    gate_weight,
    up_weight,
    down_weight,
):
    groups, mine = lax.axis_size("sp"), lax.axis_index("sp")
    chips = lax.axis_size("tp") // 2
    mixer_out = mixer(query_input, key_input, retrieved_content_matrix, gate_input, log_decay)
    token_major = lax.all_to_all(mixer_out, "tp", split_axis=1, concat_axis=0, tiled=True)
    projected = lax.dot_general(
        token_major, out_weight, (((0,), (0,)), ((), ())), preferred_element_type=jnp.float32
    )
    stream = residual.astype(jnp.float32) + projected
    scale = lax.rsqrt(jnp.mean(stream * stream, axis=-1, keepdims=True) + 1e-06)
    normed = (stream * scale * norm_gain.astype(jnp.float32)).astype(jnp.bfloat16)
    token_count, picks = routes.shape
    width = normed.shape[1]
    experts_all = groups * gate_weight.shape[0]
    capacity = (5 * token_count + 2 * experts_all - 1) // (2 * experts_all)

    side = jnp.concatenate([routes.astype(jnp.float32), *split_float(route_weight)], axis=1)
    side = jnp.pad(side.astype(jnp.bfloat16), ((0, 0), (0, 128 - side.shape[1])))
    message = row_major(jnp.concatenate([normed, side], axis=1))
    pieces = [message] + [rotate(message, "tp", 2 * step) for step in range(1, chips)]
    tokens = row_major(jnp.concatenate(pieces, axis=0))
    rows = tokens[:, :width]
    side_all = tokens[:, width:].astype(jnp.float32)
    routes_all = side_all[:, :picks].astype(jnp.int32)
    weights_all = (
        side_all[:, picks : 2 * picks]
        + side_all[:, 2 * picks : 3 * picks]
        + side_all[:, 3 * picks : 4 * picks]
    )
    relative = (routes_all - mine) % groups
    blocked = relative.reshape(chips, token_count * picks)
    matches = (blocked[:, :, None] == jnp.arange(groups)[None, None, :]).astype(jnp.float32)
    slots_before = jnp.arange(token_count * picks)
    earlier = (slots_before[:, None] > slots_before[None, :]).astype(jnp.float32)
    ranks = jnp.einsum("ij,bjg->big", earlier, matches)
    rank = jnp.sum(ranks * matches, axis=2).astype(jnp.int32)
    target = blocked * (chips * capacity) + jnp.arange(chips)[:, None] * capacity + rank
    target = target.reshape(chips * token_count, picks)
    slot_grid = jnp.arange(groups * chips * capacity)
    hits = slot_grid[:, None, None] == target[None, :, :]
    placing = jnp.sum(hits.astype(jnp.float32), axis=2).astype(jnp.bfloat16)
    taking = target[:, :, None] == slot_grid[None, None, :]
    gathering = jnp.sum(jnp.where(taking, weights_all[:, :, None], 0.0), axis=1)
    send_rows = jnp.dot(placing, rows, preferred_element_type=jnp.float32).astype(jnp.bfloat16)
    send_rows = send_rows.reshape(groups, chips * capacity, width)
    received = [send_rows[0]] + [rotate(send_rows[step], "sp", step) for step in range(1, groups)]
    own_half = jnp.concatenate(received, axis=0)
    other_half = swap_core(own_half)

    def expert(flat_rows):
        return expert_kernel(flat_rows, gate_weight[0].T, up_weight[0].T, down_weight[0])

    own_part = expert(own_half)
    other_part = swap_core(expert(other_half))
    summed = (own_part.astype(jnp.float32) + other_part.astype(jnp.float32)).astype(jnp.bfloat16)
    summed = summed.reshape(groups, chips * capacity, width)
    returned = [summed[0]] + [rotate(summed[step], "sp", -step) for step in range(1, groups)]
    flat_back = jnp.concatenate(returned, axis=0)
    high, middle, _ = split_float(gathering)
    combined = jnp.dot(
        high.astype(jnp.bfloat16), flat_back, preferred_element_type=jnp.float32
    ) + jnp.dot(middle.astype(jnp.bfloat16), flat_back, preferred_element_type=jnp.float32)
    combined = combined.reshape(chips, token_count, width)
    result = stream + combined[0]
    for step in range(1, chips):
        result = result + rotate(
            row_major(combined[step].astype(jnp.bfloat16)), "tp", -2 * step
        ).astype(jnp.float32)
    return result.astype(jnp.bfloat16)


def solution(mesh):
    placed = (
        P("tp", "sp"),
        P("tp", "sp"),
        P("tp", "sp"),
        P("tp", "sp"),
        P(None, "tp", "sp"),
        P(("sp", "tp"), None),
        P(),
        P(),
        P(("sp", "tp"), None),
        P(("sp", "tp"), None),
        P("sp", None, "tp"),
        P("sp", None, "tp"),
        P("sp", "tp", None),
    )
    return jax.shard_map(
        on_device, mesh=mesh, in_specs=placed, out_specs=P(("sp", "tp"), None), check_vma=False
    )
```
